32 devices in a mesh: ep: 16 (over z, y, core), tp: 2 (over x).
Axes of the slice: x: 2, y: 2, z: 4, core: 2. Of those that a mesh axis runs over, the one named last changes fastest.
Arguments:
- residual_in: bfloat16 [320, 1024], P('ep', 'tp'), may hold values from -64 to 64
- queries: bfloat16 [320, 512], P(('ep', 'tp')), may hold values from -6 to 6
- cache_keys: bfloat16 [320, 1024, 128], P(('ep', 'tp')), may hold values from -6 to 6
- cache_values: bfloat16 [320, 1024, 128], P(('ep', 'tp')), may hold values from -24 to 24
- lengths: int32 [320], P(('ep', 'tp')), may hold values from 256 to 1024
- stick_offset: float32 [8], replicated, may hold values from 0.5 to 6
- out_weight: bfloat16 [512, 1024], P(None, 'tp'), may hold values from -0.25 to 0.25
- norm1_gain: float32 [1024], P('tp'), may hold values from 0.3 to 3.1
- norm1_bias: float32 [1024], P('tp'), may hold values from -1.5 to 1.5
- routes: int32 [320, 6], P('ep'), may hold values from 0 to 15, all different within a row; in each aligned block of 20 rows (0 to 19, 20 to 39, ...) at most 16 rows name the same one
- route_weights: float32 [320, 6], P('ep'), may hold values from 0.1 to 0.8
- expert_gate: bfloat16 [16, 1024, 512], P('ep', None, 'tp'), may hold values from -0.1875 to 0.1875
- expert_up: bfloat16 [16, 1024, 512], P('ep', None, 'tp'), may hold values from -0.1875 to 0.1875
- expert_down: bfloat16 [16, 512, 1024], P('ep', 'tp'), may hold values from -0.25 to 0.25
- shared_gate: bfloat16 [1024, 512], P(None, 'tp'), may hold values from -0.1875 to 0.1875
- shared_up: bfloat16 [1024, 512], P(None, 'tp'), may hold values from -0.1875 to 0.1875
- shared_down: bfloat16 [512, 1024], P('tp'), may hold values from -0.25 to 0.25
- norm2_gain: float32 [1024], P('tp'), may hold values from 0.1 to 1.9
- norm2_bias: float32 [1024], P('tp'), may hold values from -1.5 to 1.5
Outputs:
- layer_out: bfloat16 [320, 1024], P('ep', 'tp')
The draws below stay inside these ranges and needn't reach their ends.
Inputs may be any that keep to these rules, and one draw needn't show every extreme that they name: `routes`: each row names 6 different experts; among the rows of one index of ep no expert is named more than 16 times.
All inputs are finite; a program needn't handle non-finite values.
Results may differ from the reference program's by a relative error of at most 0.0095.
Values may be sent and summed in bfloat16 or wider, within the bound.
A program may use at most 64 MiB of HBM per device.

```python
import math
import jax
import jax.numpy as jnp
import numpy as np
from jax import lax

D = 1024
H = 8
HD = 64
KVH = 2
CACHE = 1024
FE = 512
FS = 512
TOPK = 6
SEQ_DEV = 20
SEQS = 320
EXPERTS = 16
CAP = 16
FE_DEV = 256
N_EP = 16
N_TP = 2


def draw_residual_in(key, part):
    key_entries, key_scale = jax.random.split(key, 2)
    places = jnp.arange(D, dtype=jnp.float32) / D
    column_scale = jnp.exp(1.4 * places) * jax.random.uniform(key_scale, (D,), jnp.float32, 0.6, 1.5)
    entries = jnp.clip(jax.random.normal(key_entries, (SEQS, D), jnp.float32), -5.0, 5.0)
    return (entries * column_scale).astype(jnp.bfloat16)


def draw_norm1_gain(key, part):
    places = jnp.arange(D, dtype=jnp.float32) / D
    roughness = jax.random.uniform(key, (D,), jnp.float32, 0.8, 1.25)
    rising = 0.5 * jnp.exp(1.4 * places)
    return rising * roughness


def touch_ends(values, stream_key, low, high):
    spot = [jax.random.randint(jax.random.fold_in(stream_key, axis), (), 0, length) for axis, length in enumerate(values.shape)]
    main_axis = values.shape.index(max(values.shape))
    neighbour = spot[:main_axis] + [(spot[main_axis] + 1) % values.shape[main_axis]] + spot[main_axis + 1:]
    return values.at[tuple(spot)].set(low).at[tuple(neighbour)].set(high)


def levels(rng, extent, shards, smallest, top_value):
    level = 1.0
    for dim, blocks in shards:
        draws = jax.random.uniform(jax.random.fold_in(jax.random.fold_in(rng, 6), dim), (blocks,), jnp.float32, smallest / len(shards), top_value / len(shards))
        level = level * jnp.repeat(jnp.exp(draws), extent[dim] // blocks).reshape((-1,) + (1,) * (len(extent) - 1 - dim))
    return level


def routed_block(rng, own, number, rows, number_of, top, most, lean):
    order = jax.random.permutation(rng, number_of)
    heavy_load, usual = portions_of(number_of, rows * top, most, lean, True), portions_of(number_of, rows * top, most, lean, False)
    places = jnp.arange(number_of)

    def named(sizes, rotation):
        used = int((sizes > 0).sum())
        fixed = max(1, used // 4)
        shifted = fixed + (places - fixed + rotation * (used - fixed)) % max(1, number_of - fixed)
        return jnp.zeros((number_of,), jnp.int32).at[order[jnp.where(places < fixed, places, shifted)]].set(jnp.asarray(sizes, jnp.int32))

    sizes = jnp.where(number % 4 == 0, named(heavy_load, number // 4), named(usual, number - number // 4 - 1))
    mixed = jax.random.permutation(jax.random.fold_in(own, 3), number_of)
    donor, receiver = mixed[0:number_of // 2 * 2:2], mixed[1:number_of // 2 * 2:2]
    slack = jnp.minimum(sizes[donor] - 1, most - sizes[receiver]) // 2
    slack = jnp.where((donor == order[0]) | (receiver == order[0]) | (sizes[receiver] == 0), 0, jnp.maximum(slack, 0))
    shifted = jax.random.randint(jax.random.fold_in(own, 4), (number_of // 2,), 0, 1 << 20) % (slack + 1)
    sizes = sizes.at[donor].add(-shifted).at[receiver].add(shifted)
    items = jnp.searchsorted(jnp.cumsum(sizes), jnp.arange(rows * top), side="right").astype(jnp.int32)
    listing = items.reshape(top, rows).T
    listing = listing[jax.random.permutation(jax.random.fold_in(own, 1), rows)]
    rotation = jax.random.randint(jax.random.fold_in(own, 2), (rows, 1), 0, top)
    return jnp.take_along_axis(listing, (jnp.arange(top)[None, :] + rotation) % top, axis=1)


def portions_of(number_of, total, most, slope, full):
    loads = [(1 << 20) // math.isqrt(rank ** slope) + 1 for rank in range(1, number_of + 1)]
    largest = most if full else min(most, max(-(-total // number_of), total * loads[0] // sum(loads)))
    least = 1 if total - largest >= number_of - 1 else 0
    counts, rest = [largest] + [least] * (number_of - 1), total - largest - least * (number_of - 1)
    while rest > 0:
        movable = [i for i in range(1, number_of) if counts[i] < largest] or [i for i in range(1, number_of) if counts[i] < most]
        pool, budget = sum([loads[i] for i in movable]), rest
        for i in movable:
            addition = min(most - counts[i], max(1, budget * loads[i] // pool), rest)
            counts[i] = counts[i] + addition
            rest = rest - addition
    return np.array(counts)


def noise(rng, extent, deviation, reach, cuts=(), kind=jnp.bfloat16):
    level = levels(rng, extent, cuts, -0.22, 0.18) if cuts else 1.0
    drawn = jax.random.normal(rng, extent, jnp.float32) * deviation * level
    return jnp.minimum(jnp.maximum(drawn, -reach), reach).astype(kind)


def setup_inputs(seed: int = 0) -> dict:
    key_list = jax.random.split(jax.random.key(seed), 20)
    residual_in = draw_residual_in(jax.random.fold_in(key_list[19], 71), 0)
    queries = noise(key_list[1], (SEQS, H * HD), 1.0, 6.0, ((0, 32),))
    cache_keys = noise(key_list[2], (SEQS, CACHE, KVH * HD), 1.0, 6.0, ((0, 32),))
    cache_values = noise(key_list[3], (SEQS, CACHE, KVH * HD), 4.0, 24.0, ((0, 32),))
    lengths = touch_ends(jax.random.randint(key_list[4], (SEQS,), CACHE // 4, CACHE + 1), jax.random.fold_in(key_list[4], 1), CACHE // 4, CACHE).astype(jnp.int32)
    stick_offset = jnp.clip(jnp.exp(jax.random.uniform(key_list[5], (H,), jnp.float32, math.log(0.5), math.log(6.0))), 0.5, 6.0)
    out_weight = noise(key_list[6], (H * HD, D), (H * HD) ** -0.5, 0.25, ((1, 2),))
    norm1_gain = draw_norm1_gain(jax.random.fold_in(key_list[19], 71), 0)
    norm1_bias = noise(key_list[8], (D,), 0.3, 1.5, ((0, 2),), jnp.float32)
    routes_keys = jax.random.split(jax.random.fold_in(key_list[9], 1), SEQS // SEQ_DEV)
    routes_turns = jax.random.permutation(jax.random.fold_in(key_list[9], 3), SEQS // SEQ_DEV)
    routes = jax.vmap(lambda own, number: routed_block(jax.random.fold_in(key_list[9], 2), own, number, SEQ_DEV, EXPERTS, TOPK, CAP, 2))(routes_keys, routes_turns).reshape((SEQS, TOPK))
    route_weights = jnp.clip(0.1 + 0.7 * jax.random.uniform(key_list[10], (SEQS, TOPK), jnp.float32) ** levels(key_list[10], (SEQS, TOPK), ((0, 16),), -0.2, 0.2), 0.1, 0.8)
    expert_gate = noise(key_list[11], (EXPERTS, D, FE), D ** -0.5, 0.1875, ((0, 16), (2, 2)))
    expert_up = noise(key_list[12], (EXPERTS, D, FE), D ** -0.5, 0.1875, ((0, 16), (2, 2)))
    expert_down = noise(key_list[13], (EXPERTS, FE, D), FE ** -0.5, 0.25, ((0, 16), (1, 2)))
    shared_gate = noise(key_list[14], (D, FS), D ** -0.5, 0.1875, ((1, 2),))
    shared_up = noise(key_list[15], (D, FS), D ** -0.5, 0.1875, ((1, 2),))
    shared_down = noise(key_list[16], (FS, D), FS ** -0.5, 0.25, ((0, 2),))
    norm2_gain = jnp.clip(1.0 + 0.18 * jax.random.normal(key_list[17], (D,), jnp.float32), 0.1, 1.9)
    norm2_bias = noise(key_list[18], (D,), 0.3, 1.5, ((0, 2),), jnp.float32)
    return dict(residual_in=residual_in, queries=queries, cache_keys=cache_keys, cache_values=cache_values, lengths=lengths, stick_offset=stick_offset, out_weight=out_weight, norm1_gain=norm1_gain, norm1_bias=norm1_bias, routes=routes, route_weights=route_weights, expert_gate=expert_gate, expert_up=expert_up, expert_down=expert_down, shared_gate=shared_gate, shared_up=shared_up, shared_down=shared_down, norm2_gain=norm2_gain, norm2_bias=norm2_bias)


RESIDUAL_SCALE = 2.0 ** 0.25
EPSILON = 1e-05

def normalize(totals, squares, entries, values, scales, shifts):
    centre = totals / entries
    spread = squares / entries - centre * centre
    return (values - centre) * lax.rsqrt(spread + EPSILON) * scales + shifts

def stick_read(queries, keys_block, values_block, lengths, offsets):
    seq_count = queries.shape[0]
    grouped = H // KVH
    query_heads = queries.astype(jnp.float32).reshape(seq_count, KVH, grouped, HD)
    key_heads = keys_block.astype(jnp.float32).reshape(seq_count, CACHE, KVH, HD)
    value_heads = values_block.astype(jnp.float32).reshape(seq_count, CACHE, KVH, HD)
    scores = jnp.einsum('sgjd,slgd->sgjl', query_heads, key_heads) * HD ** (-0.5)
    scores = scores - offsets.reshape(1, KVH, grouped, 1)
    live_mask = (jnp.arange(CACHE)[None, :] < lengths[:, None])[:, None, None, :]
    keep_log = jnp.where(live_mask, jax.nn.log_sigmoid(-scores), 0.0)
    after_log = lax.cumsum(keep_log, axis=3, reverse=True) - keep_log
    weights = jnp.where(live_mask, jnp.exp(jax.nn.log_sigmoid(scores) + after_log), 0.0)
    weights = lax.optimization_barrier(weights.astype(jnp.bfloat16)).astype(jnp.float32)
    mixed = jnp.einsum('sgjl,slgd->sgjd', weights, value_heads)
    return mixed.reshape(seq_count, H * HD).astype(jnp.bfloat16)

def reference(residual_in, queries, cache_keys, cache_values, lengths, stick_offset, out_weight, norm1_gain, norm1_bias, routes, route_weights, expert_gate, expert_up, expert_down, shared_gate, shared_up, shared_down, norm2_gain, norm2_bias):
    blocks = N_EP * N_TP
    per_block = SEQ_DEV // N_TP

    def read_block(members):
        return stick_read(members[0], members[1], members[2], members[3], stick_offset)
    mixed = lax.map(read_block, (queries.reshape(blocks, per_block, H * HD), cache_keys.reshape(blocks, per_block, CACHE, KVH * HD), cache_values.reshape(blocks, per_block, CACHE, KVH * HD), lengths.reshape(blocks, per_block)))
    mixed = mixed.reshape(SEQS, H * HD)
    before = RESIDUAL_SCALE * residual_in.astype(jnp.float32) + jnp.dot(mixed, out_weight, preferred_element_type=jnp.float32)
    normed = normalize(lax.optimization_barrier(jnp.sum(before, axis=1, keepdims=True)), lax.optimization_barrier(jnp.sum(before * before, axis=1, keepdims=True)), D, before, norm1_gain, norm1_bias).astype(jnp.bfloat16)
    normed = lax.optimization_barrier(normed)
    assign = SEQ_DEV * TOPK
    slots_all = EXPERTS * CAP
    chosen = routes.reshape(N_EP, assign)
    order_ids = jnp.arange(assign)
    earlier = order_ids[None, :] < order_ids[:, None]

    def slot_of(flat):
        matches = (flat[:, None] == flat[None, :]) & earlier
        return lax.optimization_barrier(jnp.sum(matches.astype(jnp.int32), axis=1))
    slot_ids = jax.vmap(slot_of)(chosen)
    targets = chosen * CAP + slot_ids
    picks = (targets[:, :, None] == jnp.arange(slots_all)[None, None, :]).astype(jnp.float32)
    picks = picks.reshape(N_EP, SEQ_DEV, TOPK, slots_all)
    dispatch = lax.optimization_barrier(jnp.sum(picks, axis=2))
    combine = lax.optimization_barrier(jnp.sum(picks * route_weights.reshape(N_EP, SEQ_DEV, TOPK, 1), axis=2))
    rows_in = jnp.einsum('gsr,gsd->grd', dispatch, normed.reshape(N_EP, SEQ_DEV, D).astype(jnp.float32), precision=lax.Precision.HIGHEST)
    rows_in = rows_in.reshape(N_EP, EXPERTS, CAP, D).transpose(1, 0, 2, 3)
    rows_in = rows_in.reshape(EXPERTS, N_EP * CAP, D).astype(jnp.bfloat16)

    def run_expert(members):
        arrived, gate_weight, up_weight, down_weight = members
        gate_part = jnp.dot(arrived, gate_weight, preferred_element_type=jnp.float32)
        up_part = jnp.dot(arrived, up_weight, preferred_element_type=jnp.float32)
        hidden = lax.optimization_barrier((jax.nn.silu(gate_part) * up_part).astype(jnp.bfloat16))
        blocked = hidden.astype(jnp.float32).reshape(N_EP * CAP, N_TP, FE_DEV)
        partial_value = jnp.einsum('rtf,tfd->trd', blocked, down_weight.astype(jnp.float32).reshape(N_TP, FE_DEV, D))
        partial_value = lax.optimization_barrier(partial_value.astype(jnp.bfloat16)).astype(jnp.float32)
        return lax.optimization_barrier(jnp.sum(partial_value, axis=0)).astype(jnp.bfloat16)
    produced = lax.map(run_expert, (rows_in, expert_gate, expert_up, expert_down))
    produced = produced.reshape(EXPERTS, N_EP, CAP, D).transpose(1, 0, 2, 3)
    produced = produced.reshape(N_EP, slots_all, D).astype(jnp.float32)
    routed = jnp.einsum('gsr,grd->gsd', combine, produced, precision=lax.Precision.HIGHEST).reshape(SEQS, D)
    shared_hidden = (jax.nn.silu(jnp.dot(normed, shared_gate, preferred_element_type=jnp.float32)) * jnp.dot(normed, shared_up, preferred_element_type=jnp.float32)).astype(jnp.bfloat16)
    shared = jnp.dot(shared_hidden, shared_down, preferred_element_type=jnp.float32)
    after = RESIDUAL_SCALE * normed.astype(jnp.float32) + routed + shared
    return normalize(lax.optimization_barrier(jnp.sum(after, axis=1, keepdims=True)), lax.optimization_barrier(jnp.sum(after * after, axis=1, keepdims=True)), D, after, norm2_gain, norm2_bias).astype(jnp.bfloat16)
```

```python
import functools

import jax
import jax.numpy as jnp
from jax import lax
from jax.experimental import pallas as pl
from jax.experimental.pallas import tpu as pltpu
from jax.sharding import PartitionSpec as P

MESH = pl.DeviceIdType.MESH
F32, BF16 = jnp.float32, jnp.bfloat16
LANES = 128
SEQ_BATCH = 5


def kernel(
    dims, resid, q, k_hbm, v_hbm, lens, offs, wout_h, g1, b1, routes, rw,
    eg_h, eu_h, ed_h, sg_h, su_h, sd_h, g2, b2, out,
    kb, vb, wout, eg, eu, ed, sg, su, sd,
    qs, os_, rstage, reads, r24, sums1, cbuf, gath, hid, ysend, yown, sibin, zsend, xin, wsend, fin, sums2,
    loc_sem, kv_sem, c_send, c_recv, cs_send, one_send, one_recv, ga_send, gx_send, gs_send, g_recv,
    s1_send, s1_recv, s2_send, s2_recv, s3_send, s3_recv,
):
    ne, rows, rp, cols = dims
    half = ne // 2
    seqs, cache, kw = kb.shape
    heads = offs.shape[0]
    hd = q.shape[1] // heads
    grouped = heads // (kw // hd)
    nblk = cache // LANES
    me, t = lax.axis_index("ep"), lax.axis_index("tp")
    c, m = lax.rem(me, 2), me // 2
    sib, peer = me + 1 - 2 * c, 1 - t
    mine = c * half + m

    def remote(src, dst, ss, rs, ep, tp):
        return pltpu.make_async_remote_copy(
            src_ref=src, dst_ref=dst, send_sem=ss, recv_sem=rs, device_id=(ep, tp), device_id_type=MESH
        )

    kv = []
    for i in range(seqs):
        kv.append((
            pltpu.make_async_copy(k_hbm.at[i], kb.at[i], kv_sem.at[0, i]),
            pltpu.make_async_copy(v_hbm.at[i], vb.at[i], kv_sem.at[1, i]),
        ))
    for lo in range(0, seqs, SEQ_BATCH):
        for pair in kv[lo:lo + SEQ_BATCH]:
            pair[0].start()
        for pair in kv[lo:lo + SEQ_BATCH]:
            pair[1].start()
    weights = [
        pltpu.make_async_copy(a, b, loc_sem.at[n])
        for n, (a, b) in enumerate((
            (wout_h, wout), (eg_h.at[0], eg), (eu_h.at[0], eu), (ed_h.at[0], ed), (sg_h, sg), (su_h, su), (sd_h, sd)
        ))
    ]
    for copy in weights:
        copy.start()

    barrier = pltpu.get_barrier_semaphore()
    for n in range(1, half):
        pl.semaphore_signal(barrier, inc=1, device_id=(2 * lax.rem(m + n, half) + c, t), device_id_type=MESH)
    pl.semaphore_signal(barrier, inc=1, device_id=(sib, t), device_id_type=MESH)
    pl.semaphore_signal(barrier, inc=1, device_id=(me, peer), device_id_type=MESH)
    pl.semaphore_wait(barrier, half + 1)

    lane_r = lax.broadcasted_iota(jnp.int32, (rows, LANES), 1)
    coef = jnp.zeros((rows, LANES), F32)
    rt, wt = routes[...], rw[...]
    for n in range(rt.shape[1]):
        coef = coef + jnp.where(lane_r == rt[:, n:n + 1], wt[:, n:n + 1], 0.0)
    cbuf[mine] = jnp.zeros((rp, LANES), F32)
    cbuf[mine, 0:rows, :] = coef
    c_copies = []
    for n in range(1, half):
        copy = remote(cbuf.at[mine], cbuf.at[mine], c_send.at[n - 1], c_recv.at[mine], 2 * lax.rem(m + n, half) + c, t)
        copy.start()
        c_copies.append(copy)

    qf = q[...].astype(F32) * hd ** (-0.5)
    lane_q = lax.broadcasted_iota(jnp.int32, (seqs, LANES), 1)
    per = LANES // hd
    for h in range(heads):
        g = h // grouped
        x = qf[:, LANES * (h // per):LANES * (h // per + 1)]
        if h % per != g:
            x = pltpu.roll(x, hd * ((g - h) % per), 1)
        qs[:, h, :] = jnp.where(lane_q // hd == g, x, 0.0)
    span = nblk * heads
    row_i = lax.broadcasted_iota(jnp.int32, (span, LANES), 0)
    pos = (row_i // heads) * LANES + lax.broadcasted_iota(jnp.int32, (span, LANES), 1)
    off = jnp.zeros((span, LANES), F32)
    for h in range(heads):
        off = jnp.where(lax.rem(row_i, heads) == h, offs[h], off)
    tri_r = lax.broadcasted_iota(jnp.int32, (LANES, 2 * LANES), 0)
    tri_c = lax.broadcasted_iota(jnp.int32, (LANES, 2 * LANES), 1)
    tri = jnp.where((tri_r > tri_c) | (tri_c >= LANES), 1.0, 0.0).astype(BF16)
    for lo in range(0, seqs, SEQ_BATCH):
        ids = range(lo, min(lo + SEQ_BATCH, seqs))
        for i in ids:
            kv[i][0].wait()
        logs, keeps, lives = [], [], []
        for i in ids:
            sc = lax.dot_general(
                qs[i].astype(BF16), kb[i], (((1,), (1,)), ((), ())), preferred_element_type=F32
            )
            s = jnp.concatenate([sc[:, LANES * j:LANES * (j + 1)] for j in range(nblk)], axis=0) - off
            live = pos < lens[i]
            tail = jnp.log(1.0 + jnp.exp(-jnp.abs(s)))
            logs.append(jnp.minimum(s, 0.0) - tail)
            keeps.append(jnp.where(live, -jnp.maximum(s, 0.0) - tail, 0.0))
            lives.append(live)
        keep = jnp.concatenate(keeps, axis=0)
        hi = keep.astype(BF16)
        low = (keep - hi.astype(F32)).astype(BF16)
        sums = jnp.dot(hi, tri, preferred_element_type=F32) + jnp.dot(low, tri, preferred_element_type=F32)
        for i in ids:
            kv[i][1].wait()
        for n, i in enumerate(ids):
            acc = jnp.zeros((heads, LANES), F32)
            parts = [None] * nblk
            for j in reversed(range(nblk)):
                a = n * span + j * heads
                b = j * heads
                w = jnp.exp(logs[n][b:b + heads] + sums[a:a + heads, :LANES] + acc)
                parts[j] = jnp.where(lives[n][b:b + heads], w, 0.0)
                acc = acc + sums[a:a + heads, LANES:]
            os_[i] = jnp.dot(
                jnp.concatenate(parts, axis=1).astype(BF16), vb[i], preferred_element_type=F32
            )
    rstage[...] = jnp.zeros_like(rstage)
    for j in range(heads // per):
        g = j * per // grouped
        pick = jnp.zeros((seqs, LANES), F32)
        for n in range(per):
            x = os_[:, j * per + n, :]
            if n != g:
                x = pltpu.roll(x, hd * ((n - g) % per), 1)
            pick = jnp.where(lane_q // hd == n, x, pick)
        rstage[0:seqs, LANES * j:LANES * (j + 1)] = pick
    reads[t] = rstage[...].astype(BF16)
    rd = remote(reads.at[t], reads.at[t], one_send.at[0], one_recv.at[0], me, peer)
    rd.start()
    r24[...] = jnp.zeros_like(r24)
    r24[0:rows, :] = resid[...].astype(F32) * 2.0**0.25
    sp = reads.shape[1]
    sel_r = lax.broadcasted_iota(jnp.int32, (rp, 2 * sp), 0)
    sel_c = lax.broadcasted_iota(jnp.int32, (rp, 2 * sp), 1)
    chosen = (sel_r == lax.rem(sel_c, sp) + seqs * (sel_c // sp)) & (lax.rem(sel_c, sp) < seqs)
    select = jnp.where(chosen, 1.0, 0.0).astype(BF16)
    weights[0].wait()
    remote(reads.at[peer], reads.at[peer], one_send.at[0], one_recv.at[0], me, peer).wait_recv()
    mixed = jnp.concatenate([reads[0], reads[1]], axis=0)
    mixed = jnp.dot(select, mixed, preferred_element_type=F32).astype(BF16)
    before = r24[...] + jnp.dot(mixed, wout[...], preferred_element_type=F32)

    lane_s = lax.broadcasted_iota(jnp.int32, (rp, LANES), 1)

    def exchange(buf, values, n):
        total = jnp.sum(values, axis=1, keepdims=True)
        square = jnp.sum(values * values, axis=1, keepdims=True)
        buf[t] = jnp.where(lane_s == 0, total, square)
        copy = remote(buf.at[t], buf.at[t], one_send.at[n], one_recv.at[n], me, peer)
        copy.start()
        remote(buf.at[peer], buf.at[peer], one_send.at[n], one_recv.at[n], me, peer).wait_recv()
        both = buf[0] + buf[1]
        centre = both[:, 0:1] / (2 * cols)
        spread = both[:, 1:2] / (2 * cols) - centre * centre
        return copy, centre, lax.rsqrt(spread + 1e-05)

    sm1, centre, inv = exchange(sums1, before, 1)
    normed = ((before - centre) * inv * g1[...] + b1[...]).astype(BF16)

    gath[t, mine] = normed
    copies = []

    def send(copy):
        copy.start()
        copies.append(copy)

    for n in range(1, half):
        send(remote(gath.at[t, mine], gath.at[t, mine], ga_send.at[n - 1], g_recv.at[t, mine],
                    2 * lax.rem(m + n, half) + c, t))
    for n in range(half):
        slot = c * half + lax.rem(m + half - n, half)
        if n > 0:
            remote(gath.at[t, slot], gath.at[t, slot], ga_send.at[0], g_recv.at[t, slot], me, peer).wait_recv()
            remote(cbuf.at[slot], cbuf.at[slot], c_send.at[0], c_recv.at[slot], me, peer).wait_recv()
        send(remote(gath.at[t, slot], gath.at[t, slot], gx_send.at[n], g_recv.at[t, slot], me, peer))
        send(remote(gath.at[t, slot], gath.at[t, slot], gs_send.at[0, n], g_recv.at[t, slot], sib, t))
        send(remote(cbuf.at[slot], cbuf.at[slot], cs_send.at[n], c_recv.at[slot], sib, t))
    for n in range(half):
        slot = c * half + lax.rem(m + half - n, half)
        remote(gath.at[peer, slot], gath.at[peer, slot], ga_send.at[0], g_recv.at[peer, slot], me, peer).wait_recv()
        send(remote(gath.at[peer, slot], gath.at[peer, slot], gs_send.at[1, n], g_recv.at[peer, slot], sib, t))
    for copy in weights[1:]:
        copy.wait()

    def swiglu(x0, x1, wg, wu):
        gp = jnp.dot(x0, wg[0:cols], preferred_element_type=F32) + jnp.dot(x1, wg[cols:], preferred_element_type=F32)
        up = jnp.dot(x0, wu[0:cols], preferred_element_type=F32) + jnp.dot(x1, wu[cols:], preferred_element_type=F32)
        return (gp * jax.nn.sigmoid(gp) * up).astype(BF16)

    shared = jnp.dot(swiglu(gath[0, mine], gath[1, mine], sg, su), sd[...], preferred_element_type=F32)
    own_rows, sib_rows = pl.ds(c * half, half), pl.ds((1 - c) * half, half)

    def expert(which):
        x0 = gath[0, which].reshape(half * rp, cols)
        x1 = gath[1, which].reshape(half * rp, cols)
        share = cbuf[which].reshape(half * rp, LANES)
        lane = lax.broadcasted_iota(jnp.int32, (half * rp, LANES), 1)
        share = jnp.sum(jnp.where(lane == me, share, 0.0), axis=1, keepdims=True)
        hidden = swiglu(x0, x1, eg, eu)
        return [
            (jnp.dot(hidden, ed[:, cols * h:cols * (h + 1)], preferred_element_type=F32) * share).reshape(half, rp, cols)
            for h in range(2)
        ]

    own = expert(own_rows)
    yown[0], yown[1] = own[0], own[1]
    yown[0, m] += shared[:, 0:cols]
    yown[1, m] += shared[:, cols:]
    for n in range(half):
        slot = (1 - c) * half + n
        for h in range(2):
            remote(gath.at[h, slot], gath.at[h, slot], ga_send.at[0], g_recv.at[h, slot], me, peer).wait_recv()
        remote(cbuf.at[slot], cbuf.at[slot], c_send.at[0], c_recv.at[slot], me, peer).wait_recv()
    other = expert(sib_rows)
    ysend[0], ysend[1] = other[0].astype(BF16), other[1].astype(BF16)
    send(remote(ysend.at[peer], sibin.at[peer], s1_send.at[0], s1_recv.at[0], sib, t))
    send(remote(ysend.at[t], sibin.at[t], s1_send.at[1], s1_recv.at[1], sib, t))
    remote(ysend.at[peer], sibin.at[peer], s1_send.at[0], s1_recv.at[0], sib, t).wait_recv()
    for n in range(half):
        j = lax.rem(m + n + 1, half)
        zsend[j] = (yown[peer, j] + sibin[peer, j].astype(F32)).astype(BF16)
        send(remote(zsend.at[j], xin.at[j], s2_send.at[n], s2_recv.at[j], me, peer))
    remote(ysend.at[t], sibin.at[t], s1_send.at[1], s1_recv.at[1], sib, t).wait_recv()
    total = 2.0**0.25 * normed.astype(F32)
    for n in range(half):
        j = lax.rem(m + n + 1, half)
        here = yown[t, j] + sibin[t, j].astype(F32)
        remote(xin.at[j], xin.at[j], s2_send.at[0], s2_recv.at[j], me, peer).wait_recv()
        here = here + xin[j].astype(F32)
        if n < half - 1:
            wsend[j] = here.astype(BF16)
            send(remote(wsend.at[j], fin.at[m], s3_send.at[n], s3_recv.at[m], 2 * j + c, t))
        else:
            total = total + here
    for n in range(1, half):
        j = lax.rem(m + half - n, half)
        remote(fin.at[j], fin.at[j], s3_send.at[0], s3_recv.at[j], me, peer).wait_recv()
        total = total + fin[j].astype(F32)
    sm2, centre, inv = exchange(sums2, total, 2)
    final = (total - centre) * inv * g2[...] + b2[...]
    out[...] = final[0:rows].astype(BF16)
    for copy in c_copies + [rd, sm1, sm2] + copies:
        copy.wait_send()


def paired(ne, *args):
    (resid, q, k, v, lens, offs, wout, g1, b1, routes, rw, eg, eu, ed, sg, su, sd, g2, b2) = args
    rows, cols = resid.shape
    rp = -(-rows // 8) * 8
    half = ne // 2
    seqs = q.shape[0]
    sp = -(-seqs // 8) * 8
    heads = offs.shape[0]
    vm, anys, sm = (pl.BlockSpec(memory_space=s) for s in (pltpu.VMEM, pl.ANY, pltpu.SMEM))
    dma = pltpu.SemaphoreType.DMA
    return pl.pallas_call(
        functools.partial(kernel, (ne, rows, rp, cols)),
        out_shape=jax.ShapeDtypeStruct((rows, cols), BF16),
        in_specs=[vm, vm, anys, anys, sm, sm, anys, vm, vm, vm, vm, anys, anys, anys, anys, anys, anys, vm, vm],
        out_specs=vm,
        scratch_shapes=[
            pltpu.VMEM(k.shape, BF16),
            pltpu.VMEM(v.shape, BF16),
            pltpu.VMEM(wout.shape, BF16),
            pltpu.VMEM(eg.shape[1:], BF16),
            pltpu.VMEM(eu.shape[1:], BF16),
            pltpu.VMEM(ed.shape[1:], BF16),
            pltpu.VMEM(sg.shape, BF16),
            pltpu.VMEM(su.shape, BF16),
            pltpu.VMEM(sd.shape, BF16),
            pltpu.VMEM((seqs, heads, LANES), F32),
            pltpu.VMEM((seqs, heads, LANES), F32),
            pltpu.VMEM((sp, q.shape[1]), F32),
            pltpu.VMEM((2, sp, q.shape[1]), BF16),
            pltpu.VMEM((rp, cols), F32),
            pltpu.VMEM((2, rp, LANES), F32),
            pltpu.VMEM((ne, rp, LANES), F32),
            pltpu.VMEM((2, ne, rp, cols), BF16),
            pltpu.VMEM((8, LANES), BF16),
            pltpu.VMEM((2, half, rp, cols), BF16),
            pltpu.VMEM((2, half, rp, cols), F32),
            pltpu.VMEM((2, half, rp, cols), BF16),
            pltpu.VMEM((half, rp, cols), BF16),
            pltpu.VMEM((half, rp, cols), BF16),
            pltpu.VMEM((half, rp, cols), BF16),
            pltpu.VMEM((half, rp, cols), BF16),
            pltpu.VMEM((2, rp, LANES), F32),
            dma((7,)), dma((2, seqs)), dma((half,)), dma((ne,)), dma((half,)), dma((3,)), dma((3,)),
            dma((half,)), dma((half,)), dma((2, half)), dma((2, ne)),
            dma((2,)), dma((2,)), dma((half,)), dma((half,)), dma((half,)), dma((half,)),
        ],
        compiler_params=pltpu.CompilerParams(
            collective_id=0, has_side_effects=True, vmem_limit_bytes=56 * 2**20
        ),
    )(resid, q, k, v, lens, offs, wout, g1.reshape(1, -1), b1.reshape(1, -1), routes, rw,
      eg, eu, ed, sg, su, sd, g2.reshape(1, -1), b2.reshape(1, -1))


H = 8
HD = 64
KVH = 2
CACHE = 1024
TOPK = 6


RESIDUAL_SCALE = 2.0**0.25
EPSILON = 1e-05


def normalize(totals, squares, entries, values, scales, shifts):
    centre = totals / entries
    spread = squares / entries - centre * centre
    return (values - centre) * lax.rsqrt(spread + EPSILON) * scales + shifts


def stick_read(queries, keys_block, values_block, lengths, offsets):
    seq_count = queries.shape[0]
    grouped = H // KVH
    query_heads = queries.reshape(seq_count, KVH, grouped, HD)
    key_heads = keys_block.reshape(seq_count, CACHE, KVH, HD)
    value_heads = values_block.reshape(seq_count, CACHE, KVH, HD)
    scores = jnp.einsum(
        "sgjd,slgd->sgjl", query_heads, key_heads, preferred_element_type=jnp.float32
    )
    scores = scores * HD ** (-0.5) - offsets.reshape(1, KVH, grouped, 1)
    live_mask = (jnp.arange(CACHE)[None, :] < lengths[:, None])[:, None, None, :]
    keep_log = jnp.where(live_mask, jax.nn.log_sigmoid(-scores), 0.0)
    after_log = lax.cumsum(keep_log, axis=3, reverse=True) - keep_log
    weights = jnp.where(live_mask, jnp.exp(jax.nn.log_sigmoid(scores) + after_log), 0.0)
    weights = weights.astype(jnp.bfloat16)
    mixed = jnp.einsum("sgjl,slgd->sgjd", weights, value_heads, preferred_element_type=jnp.float32)
    return mixed.reshape(seq_count, H * HD).astype(jnp.bfloat16)


def body(
    residual_in,
    queries,
    cache_keys,
    cache_values,
    lengths,
    stick_offset,
    out_weight,
    norm1_gain,
    norm1_bias,
    routes,
    route_weights,
    expert_gate,
    expert_up,
    expert_down,
    shared_gate,
    shared_up,
    shared_down,
    norm2_gain,
    norm2_bias,
):
    mixed = stick_read(queries, cache_keys, cache_values, lengths, stick_offset)
    attended = jnp.dot(
        lax.all_gather(mixed, "tp", axis=0, tiled=True),
        out_weight,
        preferred_element_type=jnp.float32,
    )
    before = RESIDUAL_SCALE * residual_in.astype(jnp.float32) + attended
    group_rows, columns = residual_in.shape
    full_width = columns * lax.axis_size("tp")
    totals, squares = lax.psum((jnp.sum(before, axis=1), jnp.sum(before * before, axis=1)), "tp")
    normed = normalize(
        totals[:, None], squares[:, None], full_width, before, norm1_gain, norm1_bias
    ).astype(jnp.bfloat16)
    whole = lax.all_gather(normed, "tp", axis=1, tiled=True)
    experts = lax.axis_size("ep")
    capacity = min(group_rows, 2 * ((group_rows * TOPK + experts - 1) // experts))
    slots_all = experts * capacity
    chosen = routes.reshape(-1)
    order_ids = jnp.arange(chosen.shape[0])
    matches = (chosen[:, None] == chosen[None, :]) & (order_ids[None, :] < order_ids[:, None])
    targets = chosen * capacity + jnp.sum(matches.astype(jnp.int32), axis=1)
    picks = (targets[:, None] == jnp.arange(slots_all)[None, :]).astype(jnp.float32)
    picks = picks.reshape(group_rows, TOPK, slots_all)
    dispatch = jnp.sum(picks, axis=1).astype(jnp.bfloat16)
    combine = jnp.sum(picks * route_weights[:, :, None], axis=1)
    parcel = jnp.einsum("sr,sd->rd", dispatch, normed, preferred_element_type=jnp.float32)
    parcel = parcel.astype(jnp.bfloat16).reshape(experts, capacity, columns)
    arrived = lax.all_gather(
        lax.all_to_all(parcel, "ep", split_axis=0, concat_axis=0, tiled=True),
        "tp",
        axis=2,
        tiled=True,
    )
    gate_part = jnp.einsum(
        "ecd,df->ecf", arrived, expert_gate[0], preferred_element_type=jnp.float32
    )
    up_part = jnp.einsum("ecd,df->ecf", arrived, expert_up[0], preferred_element_type=jnp.float32)
    hidden = (jax.nn.silu(gate_part) * up_part).astype(jnp.bfloat16)
    partial_value = jnp.einsum(
        "ecf,fd->ecd", hidden, expert_down[0], preferred_element_type=jnp.float32
    )
    summed = lax.psum_scatter(
        partial_value.astype(jnp.bfloat16), "tp", scatter_dimension=2, tiled=True
    )
    returned = lax.all_to_all(summed, "ep", split_axis=0, concat_axis=0, tiled=True)
    routed = jnp.dot(
        combine,
        returned.reshape(slots_all, columns).astype(jnp.float32),
        precision=lax.Precision.HIGHEST,
    )
    shared_hidden = (
        jax.nn.silu(jnp.dot(whole, shared_gate, preferred_element_type=jnp.float32))
        * jnp.dot(whole, shared_up, preferred_element_type=jnp.float32)
    ).astype(jnp.bfloat16)
    shared_term = jnp.dot(shared_hidden, shared_down, preferred_element_type=jnp.float32)
    shared = lax.psum_scatter(
        shared_term.astype(jnp.bfloat16), "tp", scatter_dimension=1, tiled=True
    ).astype(jnp.float32)
    after = RESIDUAL_SCALE * normed.astype(jnp.float32) + routed + shared
    final_totals, final_squares = lax.psum(
        (jnp.sum(after, axis=1), jnp.sum(after * after, axis=1)), "tp"
    )
    return normalize(
        final_totals[:, None], final_squares[:, None], full_width, after, norm2_gain, norm2_bias
    ).astype(jnp.bfloat16)


def solution(mesh):
    in_specs = (
        P("ep", "tp"),
        P(("ep", "tp"), None),
        P(("ep", "tp"), None, None),
        P(("ep", "tp"), None, None),
        P(("ep", "tp")),
        P(),
        P(None, "tp"),
        P("tp"),
        P("tp"),
        P("ep", None),
        P("ep", None),
        P("ep", None, "tp"),
        P("ep", None, "tp"),
        P("ep", "tp", None),
        P(None, "tp"),
        P(None, "tp"),
        P("tp", None),
        P("tp"),
        P("tp"),
    )
    out_specs = P("ep", "tp")
    ne = mesh.shape["ep"]
    fits = mesh.shape["tp"] == 2 and ne % 2 == 0 and ne <= LANES // 4
    step = functools.partial(paired, ne) if fits else body
    return jax.shard_map(step, mesh=mesh, in_specs=in_specs, out_specs=out_specs, check_vma=False)
```

```python
import functools

import jax
import jax.numpy as jnp
from jax import lax
from jax.experimental import pallas as pl
from jax.experimental.pallas import tpu as pltpu
from jax.sharding import PartitionSpec as P

MESH = pl.DeviceIdType.MESH
F32, BF16 = jnp.float32, jnp.bfloat16
LANES = 128
SEQ_BATCH = 10


def kernel(
    dims, resid_h, q_h, k_hbm, v_hbm, lens, offs, wout_h, g1_h, b1_h, routes_h, rw_h,
    eg_h, eu_h, ed_h, sg_h, su_h, sd_h, g2_h, b2_h, out,
    resid, q, g1, b1, routes, rw, g2, b2, rpad, wpad, small_sem,
    kb, vb, wout, eg, eu, ed, sg, su, sd,
    qs, os_, rstage, reads, r24, sums1, cbuf, gath, ysend, yown, sibin, zsend, xin, wsend, fin, sums2,
    loc_sem, kv_sem, c_send, c_recv, cs_send, one_send, one_recv, ga_send, gx_send, gs_send, g_recv,
    s1_send, s1_recv, s2_send, s2_recv, s3_send, s3_recv,
):
    ne, rows, rp, cols = dims
    half = ne // 2
    seqs, cache, kw = kb.shape
    heads = offs.shape[0]
    hd = q.shape[1] // heads
    grouped = heads // (kw // hd)
    nblk = cache // LANES
    me, t = lax.axis_index("ep"), lax.axis_index("tp")
    c, m = lax.rem(me, 2), me // 2
    sib, peer = me + 1 - 2 * c, 1 - t

    def mate(n):
        j, bit = 0, 1
        while bit < half:
            b = lax.rem(m // bit, 2)
            j = j + bit * ((1 - b) if n & bit else b)
            bit *= 2
        return j

    mine = c * half + m

    def remote(src, dst, ss, rs, ep, tp):
        return pltpu.make_async_remote_copy(
            src_ref=src, dst_ref=dst, send_sem=ss, recv_sem=rs, device_id=(ep, tp), device_id_type=MESH
        )

    barrier = pltpu.get_barrier_semaphore()
    for n in range(1, half):
        pl.semaphore_signal(barrier, inc=1, device_id=(2 * mate(n) + c, t), device_id_type=MESH)
    pl.semaphore_signal(barrier, inc=1, device_id=(sib, t), device_id_type=MESH)
    pl.semaphore_signal(barrier, inc=1, device_id=(me, peer), device_id_type=MESH)

    small = [
        pltpu.make_async_copy(a, b, small_sem.at[n])
        for n, (a, b) in enumerate((
            (routes_h, routes), (rw_h, rw), (q_h, q), (resid_h, resid), (g1_h, g1), (b1_h, b1), (g2_h, g2), (b2_h, b2)
        ))
    ]
    for copy in small:
        copy.start()
    kv = []
    for i in range(seqs):
        kv.append((
            pltpu.make_async_copy(k_hbm.at[i], kb.at[i], kv_sem.at[0, i]),
            pltpu.make_async_copy(v_hbm.at[i], vb.at[i], kv_sem.at[1, i]),
        ))
    for lo in range(0, seqs, SEQ_BATCH):
        for pair in kv[lo:lo + SEQ_BATCH]:
            pair[0].start()
        for pair in kv[lo:lo + SEQ_BATCH]:
            pair[1].start()
    weights = [
        pltpu.make_async_copy(a, b, loc_sem.at[n])
        for n, (a, b) in enumerate((
            (wout_h, wout), (eg_h.at[0], eg), (eu_h.at[0], eu), (ed_h.at[0], ed), (sg_h, sg), (su_h, su), (sd_h, sd)
        ))
    ]
    for copy in weights:
        copy.start()


    small[2].wait()
    qf = q[...].astype(F32) * hd ** (-0.5)
    lane_q = lax.broadcasted_iota(jnp.int32, (seqs, LANES), 1)
    per = LANES // hd
    for h in range(heads):
        g = h // grouped
        x = qf[:, LANES * (h // per):LANES * (h // per + 1)]
        if h % per != g:
            x = pltpu.roll(x, hd * ((g - h) % per), 1)
        qs[:, h, :] = jnp.where(lane_q // hd == g, x, 0.0)
    span = nblk * heads
    row_i = lax.broadcasted_iota(jnp.int32, (span, LANES), 0)
    pos = (row_i // heads) * LANES + lax.broadcasted_iota(jnp.int32, (span, LANES), 1)
    off = jnp.zeros((span, LANES), F32)
    for h in range(heads):
        off = jnp.where(lax.rem(row_i, heads) == h, offs[h], off)
    tri_r = lax.broadcasted_iota(jnp.int32, (LANES, 2 * LANES), 0)
    tri_c = lax.broadcasted_iota(jnp.int32, (LANES, 2 * LANES), 1)
    tri = jnp.where((tri_r > tri_c) | (tri_c >= LANES), 1.0, 0.0).astype(BF16)
    for lo in range(0, seqs, SEQ_BATCH):
        ids = range(lo, min(lo + SEQ_BATCH, seqs))
        for i in ids:
            kv[i][0].wait()
        logs, keeps, lives = [], [], []
        for i in ids:
            sc = lax.dot_general(
                qs[i].astype(BF16), kb[i], (((1,), (1,)), ((), ())), preferred_element_type=F32
            )
            s = jnp.concatenate([sc[:, LANES * j:LANES * (j + 1)] for j in range(nblk)], axis=0) - off
            live = pos < lens[i]
            tail = jnp.log(1.0 + jnp.exp(-jnp.abs(s)))
            logs.append(jnp.minimum(s, 0.0) - tail)
            keeps.append(jnp.where(live, -jnp.maximum(s, 0.0) - tail, 0.0))
            lives.append(live)
        keep = jnp.concatenate(keeps, axis=0)
        hi = keep.astype(BF16)
        low = (keep - hi.astype(F32)).astype(BF16)
        sums = jnp.dot(hi, tri, preferred_element_type=F32) + jnp.dot(low, tri, preferred_element_type=F32)
        for i in ids:
            kv[i][1].wait()
        for n, i in enumerate(ids):
            acc = jnp.zeros((heads, LANES), F32)
            parts = [None] * nblk
            for j in reversed(range(nblk)):
                a = n * span + j * heads
                b = j * heads
                w = jnp.exp(logs[n][b:b + heads] + sums[a:a + heads, :LANES] + acc)
                parts[j] = jnp.where(lives[n][b:b + heads], w, 0.0)
                acc = acc + sums[a:a + heads, LANES:]
            os_[i] = jnp.dot(
                jnp.concatenate(parts, axis=1).astype(BF16), vb[i], preferred_element_type=F32
            )
    rstage[...] = jnp.zeros_like(rstage)
    for j in range(heads // per):
        g = j * per // grouped
        pick = jnp.zeros((seqs, LANES), F32)
        for n in range(per):
            x = os_[:, j * per + n, :]
            if n != g:
                x = pltpu.roll(x, hd * ((n - g) % per), 1)
            pick = jnp.where(lane_q // hd == n, x, pick)
        rstage[0:seqs, LANES * j:LANES * (j + 1)] = pick
    for copy in small[:2] + small[3:]:
        copy.wait()
    expert_of = lax.broadcasted_iota(jnp.int32, (LANES, LANES), 0)
    coef = jnp.zeros((LANES, LANES), F32)
    topk = routes.shape[0]
    rpad[...] = jnp.full(rpad.shape, -1, jnp.int32)
    wpad[...] = jnp.zeros(wpad.shape, F32)
    rpad[0:topk, 0:rows] = routes[...]
    wpad[0:topk, 0:rows] = rw[...]
    rt, wt = rpad[...], wpad[...]
    for n in range(topk):
        coef = coef + jnp.where(expert_of == rt[n:n + 1, :], wt[n:n + 1, :], 0.0)
    cbuf[mine] = coef.T[0:rp]
    pl.semaphore_wait(barrier, half + 1)
    reads[t] = rstage[...].astype(BF16)
    rd = remote(reads.at[t], reads.at[t], one_send.at[0], one_recv.at[0], me, peer)
    rd.start()
    c_copies = []
    for n in range(1, half):
        copy = remote(cbuf.at[mine], cbuf.at[mine], c_send.at[n - 1], c_recv.at[mine], 2 * mate(n) + c, t)
        copy.start()
        c_copies.append(copy)
    r24[...] = jnp.zeros_like(r24)
    r24[0:rows, :] = resid[...].astype(F32) * 2.0**0.25
    sp = reads.shape[1]
    sel_r = lax.broadcasted_iota(jnp.int32, (rp, 2 * sp), 0)
    sel_c = lax.broadcasted_iota(jnp.int32, (rp, 2 * sp), 1)
    chosen = (sel_r == lax.rem(sel_c, sp) + seqs * (sel_c // sp)) & (lax.rem(sel_c, sp) < seqs)
    select = jnp.where(chosen, 1.0, 0.0).astype(BF16)
    weights[0].wait()
    remote(reads.at[peer], reads.at[peer], one_send.at[0], one_recv.at[0], me, peer).wait_recv()
    mixed = jnp.concatenate([reads[0], reads[1]], axis=0)
    mixed = jnp.dot(select, mixed, preferred_element_type=F32).astype(BF16)
    before = r24[...] + jnp.dot(mixed, wout[...], preferred_element_type=F32)

    lane_s = lax.broadcasted_iota(jnp.int32, (rp, LANES), 1)

    def exchange(buf, values, n):
        total = jnp.sum(values, axis=1, keepdims=True)
        square = jnp.sum(values * values, axis=1, keepdims=True)
        buf[t] = jnp.where(lane_s == 0, total, square)
        copy = remote(buf.at[t], buf.at[t], one_send.at[n], one_recv.at[n], me, peer)
        copy.start()
        remote(buf.at[peer], buf.at[peer], one_send.at[n], one_recv.at[n], me, peer).wait_recv()
        both = buf[0] + buf[1]
        centre = both[:, 0:1] / (2 * cols)
        spread = both[:, 1:2] / (2 * cols) - centre * centre
        return copy, centre, lax.rsqrt(spread + 1e-05)

    sm1, centre, inv = exchange(sums1, before, 1)
    normed = ((before - centre) * inv * g1[...] + b1[...]).astype(BF16)

    gath[t, mine] = normed
    copies = []

    def send(copy):
        copy.start()
        copies.append(copy)

    for n in range(1, half):
        send(remote(gath.at[t, mine], gath.at[t, mine], ga_send.at[n - 1], g_recv.at[t, mine],
                    2 * mate(n) + c, t))
    for n in range(half):
        slot = c * half + mate(n)
        if n > 0:
            remote(gath.at[t, slot], gath.at[t, slot], ga_send.at[0], g_recv.at[t, slot], me, peer).wait_recv()
            remote(cbuf.at[slot], cbuf.at[slot], c_send.at[0], c_recv.at[slot], me, peer).wait_recv()
        send(remote(gath.at[t, slot], gath.at[t, slot], gx_send.at[n], g_recv.at[t, slot], me, peer))
        send(remote(gath.at[t, slot], gath.at[t, slot], gs_send.at[0, n], g_recv.at[t, slot], sib, t))
        send(remote(cbuf.at[slot], cbuf.at[slot], cs_send.at[n], c_recv.at[slot], sib, t))
    for n in range(half):
        slot = c * half + mate(n)
        remote(gath.at[peer, slot], gath.at[peer, slot], ga_send.at[0], g_recv.at[peer, slot], me, peer).wait_recv()
        send(remote(gath.at[peer, slot], gath.at[peer, slot], gs_send.at[1, n], g_recv.at[peer, slot], sib, t))
    for copy in weights[1:]:
        copy.wait()

    def swiglu(x0, x1, wg, wu):
        gp = jnp.dot(x0, wg[0:cols], preferred_element_type=F32) + jnp.dot(x1, wg[cols:], preferred_element_type=F32)
        up = jnp.dot(x0, wu[0:cols], preferred_element_type=F32) + jnp.dot(x1, wu[cols:], preferred_element_type=F32)
        return (gp * jax.nn.sigmoid(gp) * up).astype(BF16)

    shared = jnp.dot(swiglu(gath[0, mine], gath[1, mine], sg, su), sd[...], preferred_element_type=F32)
    def expert(slots):
        def rows_of(buf):
            return jnp.concatenate([buf[s] for s in slots], axis=0)

        share = rows_of(cbuf)
        lane = lax.broadcasted_iota(jnp.int32, share.shape, 1)
        share = jnp.sum(jnp.where(lane == me, share, 0.0), axis=1, keepdims=True)
        hidden = swiglu(rows_of(gath.at[0]), rows_of(gath.at[1]), eg, eu)
        for h in (peer, t):
            part = jnp.dot(hidden, ed[:, pl.ds(pl.multiple_of(h * cols, cols), cols)], preferred_element_type=F32)
            yield h, (part * share).reshape(len(slots), rp, cols)

    order = [mate(n) for n in reversed(range(half))]
    for h, part in expert([c * half + n for n in range(half)]):
        yown[h] = part
    yown[0, m] += shared[:, 0:cols]
    yown[1, m] += shared[:, cols:]
    cut = (half + 1) // 2
    for part_id, (lo, hi) in enumerate(((0, cut), (cut, half))):
        slots = [(1 - c) * half + j for j in order[lo:hi]]
        for slot in slots:
            for h in range(2):
                remote(gath.at[h, slot], gath.at[h, slot], ga_send.at[0], g_recv.at[h, slot], me, peer).wait_recv()
            remote(cbuf.at[slot], cbuf.at[slot], c_send.at[0], c_recv.at[slot], me, peer).wait_recv()
        for half_id, (h, part) in enumerate(expert(slots)):
            ysend[h, lo:hi] = part.astype(BF16)
            send(remote(ysend.at[h, pl.ds(lo, hi - lo)], sibin.at[h, pl.ds(lo, hi - lo)],
                        s1_send.at[half_id, part_id], s1_recv.at[half_id, part_id], sib, t))

    def arrived(half_id, h, n):
        for part_id, (lo, hi) in enumerate(((0, cut), (cut, half))):
            if n == lo:
                ref = sibin.at[h, pl.ds(lo, hi - lo)]
                remote(ref, ref, s1_send.at[0, 0], s1_recv.at[half_id, part_id], sib, t).wait_recv()

    for n, j in enumerate(order):
        arrived(0, peer, n)
        zsend[n] = (yown[peer, j] + sibin[peer, n].astype(F32)).astype(BF16)
        send(remote(zsend.at[n], xin.at[n], s2_send.at[n], s2_recv.at[n], me, peer))
    total = 2.0**0.25 * normed.astype(F32)
    for n, j in enumerate(order):
        arrived(1, t, n)
        here = yown[t, j] + sibin[t, n].astype(F32)
        remote(xin.at[n], xin.at[n], s2_send.at[0], s2_recv.at[n], me, peer).wait_recv()
        here = here + xin[n].astype(F32)
        if n < half - 1:
            wsend[n] = here.astype(BF16)
            send(remote(wsend.at[n], fin.at[m], s3_send.at[n], s3_recv.at[m], 2 * j + c, t))
        else:
            total = total + here
    for n in range(1, half):
        j = mate(n)
        remote(fin.at[j], fin.at[j], s3_send.at[0], s3_recv.at[j], me, peer).wait_recv()
        total = total + fin[j].astype(F32)
    sm2, centre, inv = exchange(sums2, total, 2)
    final = (total - centre) * inv * g2[...] + b2[...]
    out[...] = final[0:rows].astype(BF16)
    for copy in c_copies + [rd, sm1, sm2] + copies:
        copy.wait_send()


def paired(ne, *args):
    (resid, q, k, v, lens, offs, wout, g1, b1, routes, rw, eg, eu, ed, sg, su, sd, g2, b2) = args
    rows, cols = resid.shape
    rp = -(-rows // 8) * 8
    half = ne // 2
    seqs = q.shape[0]
    sp = -(-seqs // 8) * 8
    heads = offs.shape[0]
    vm, anys, sm = (pl.BlockSpec(memory_space=s) for s in (pltpu.VMEM, pl.ANY, pltpu.SMEM))
    dma = pltpu.SemaphoreType.DMA
    return pl.pallas_call(
        functools.partial(kernel, (ne, rows, rp, cols)),
        out_shape=jax.ShapeDtypeStruct((rows, cols), BF16),
        in_specs=[anys] * 4 + [sm] * 2 + [anys] * 13,
        out_specs=vm,
        scratch_shapes=[
            pltpu.VMEM(resid.shape, BF16),
            pltpu.VMEM(q.shape, BF16),
            pltpu.VMEM((1, cols), F32),
            pltpu.VMEM((1, cols), F32),
            pltpu.VMEM(routes.shape[::-1], jnp.int32),
            pltpu.VMEM(rw.shape[::-1], F32),
            pltpu.VMEM((1, cols), F32),
            pltpu.VMEM((1, cols), F32),
            pltpu.VMEM((-(-routes.shape[1] // 8) * 8, LANES), jnp.int32),
            pltpu.VMEM((-(-routes.shape[1] // 8) * 8, LANES), F32),
            dma((8,)),
            pltpu.VMEM(k.shape, BF16),
            pltpu.VMEM(v.shape, BF16),
            pltpu.VMEM(wout.shape, BF16),
            pltpu.VMEM(eg.shape[1:], BF16),
            pltpu.VMEM(eu.shape[1:], BF16),
            pltpu.VMEM(ed.shape[1:], BF16),
            pltpu.VMEM(sg.shape, BF16),
            pltpu.VMEM(su.shape, BF16),
            pltpu.VMEM(sd.shape, BF16),
            pltpu.VMEM((seqs, heads, LANES), F32),
            pltpu.VMEM((seqs, heads, LANES), F32),
            pltpu.VMEM((sp, q.shape[1]), F32),
            pltpu.VMEM((2, sp, q.shape[1]), BF16),
            pltpu.VMEM((rp, cols), F32),
            pltpu.VMEM((2, rp, LANES), F32),
            pltpu.VMEM((ne, rp, LANES), F32),
            pltpu.VMEM((2, ne, rp, cols), BF16),
            pltpu.VMEM((2, half, rp, cols), BF16),
            pltpu.VMEM((2, half, rp, cols), F32),
            pltpu.VMEM((2, half, rp, cols), BF16),
            pltpu.VMEM((half, rp, cols), BF16),
            pltpu.VMEM((half, rp, cols), BF16),
            pltpu.VMEM((half, rp, cols), BF16),
            pltpu.VMEM((half, rp, cols), BF16),
            pltpu.VMEM((2, rp, LANES), F32),
            dma((7,)), dma((2, seqs)), dma((half,)), dma((ne,)), dma((half,)), dma((3,)), dma((3,)),
            dma((half,)), dma((half,)), dma((2, half)), dma((2, ne)),
            dma((2, 2)), dma((2, 2)), dma((half,)), dma((half,)), dma((half,)), dma((half,)),
        ],
        compiler_params=pltpu.CompilerParams(
            collective_id=0, has_side_effects=True, vmem_limit_bytes=56 * 2**20
        ),
    )(resid, q, k, v, lens, offs, wout, g1.reshape(1, -1), b1.reshape(1, -1), routes.T, rw.T,
      eg, eu, ed, sg, su, sd, g2.reshape(1, -1), b2.reshape(1, -1))


H = 8
HD = 64
KVH = 2
CACHE = 1024
TOPK = 6


RESIDUAL_SCALE = 2.0**0.25
EPSILON = 1e-05


def normalize(totals, squares, entries, values, scales, shifts):
    centre = totals / entries
    spread = squares / entries - centre * centre
    return (values - centre) * lax.rsqrt(spread + EPSILON) * scales + shifts


def stick_read(queries, keys_block, values_block, lengths, offsets):
    seq_count = queries.shape[0]
    grouped = H // KVH
    query_heads = queries.reshape(seq_count, KVH, grouped, HD)
    key_heads = keys_block.reshape(seq_count, CACHE, KVH, HD)
    value_heads = values_block.reshape(seq_count, CACHE, KVH, HD)
    scores = jnp.einsum(
        "sgjd,slgd->sgjl", query_heads, key_heads, preferred_element_type=jnp.float32
    )
    scores = scores * HD ** (-0.5) - offsets.reshape(1, KVH, grouped, 1)
    live_mask = (jnp.arange(CACHE)[None, :] < lengths[:, None])[:, None, None, :]
    keep_log = jnp.where(live_mask, jax.nn.log_sigmoid(-scores), 0.0)
    after_log = lax.cumsum(keep_log, axis=3, reverse=True) - keep_log
    weights = jnp.where(live_mask, jnp.exp(jax.nn.log_sigmoid(scores) + after_log), 0.0)
    weights = weights.astype(jnp.bfloat16)
    mixed = jnp.einsum("sgjl,slgd->sgjd", weights, value_heads, preferred_element_type=jnp.float32)
    return mixed.reshape(seq_count, H * HD).astype(jnp.bfloat16)


def body(
    residual_in,
    queries,
    cache_keys,
    cache_values,
    lengths,
    stick_offset,
    out_weight,
    norm1_gain,
    norm1_bias,
    routes,
    route_weights,
    expert_gate,
    expert_up,
    expert_down,
    shared_gate,
    shared_up,
    shared_down,
    norm2_gain,
    norm2_bias,
):
    mixed = stick_read(queries, cache_keys, cache_values, lengths, stick_offset)
    attended = jnp.dot(
        lax.all_gather(mixed, "tp", axis=0, tiled=True),
        out_weight,
        preferred_element_type=jnp.float32,
    )
    before = RESIDUAL_SCALE * residual_in.astype(jnp.float32) + attended
    group_rows, columns = residual_in.shape
    full_width = columns * lax.axis_size("tp")
    totals, squares = lax.psum((jnp.sum(before, axis=1), jnp.sum(before * before, axis=1)), "tp")
    normed = normalize(
        totals[:, None], squares[:, None], full_width, before, norm1_gain, norm1_bias
    ).astype(jnp.bfloat16)
    whole = lax.all_gather(normed, "tp", axis=1, tiled=True)
    experts = lax.axis_size("ep")
    capacity = min(group_rows, 2 * ((group_rows * TOPK + experts - 1) // experts))
    slots_all = experts * capacity
    chosen = routes.reshape(-1)
    order_ids = jnp.arange(chosen.shape[0])
    matches = (chosen[:, None] == chosen[None, :]) & (order_ids[None, :] < order_ids[:, None])
    targets = chosen * capacity + jnp.sum(matches.astype(jnp.int32), axis=1)
    picks = (targets[:, None] == jnp.arange(slots_all)[None, :]).astype(jnp.float32)
    picks = picks.reshape(group_rows, TOPK, slots_all)
    dispatch = jnp.sum(picks, axis=1).astype(jnp.bfloat16)
    combine = jnp.sum(picks * route_weights[:, :, None], axis=1)
    parcel = jnp.einsum("sr,sd->rd", dispatch, normed, preferred_element_type=jnp.float32)
    parcel = parcel.astype(jnp.bfloat16).reshape(experts, capacity, columns)
    arrived = lax.all_gather(
        lax.all_to_all(parcel, "ep", split_axis=0, concat_axis=0, tiled=True),
        "tp",
        axis=2,
        tiled=True,
    )
    gate_part = jnp.einsum(
        "ecd,df->ecf", arrived, expert_gate[0], preferred_element_type=jnp.float32
    )
    up_part = jnp.einsum("ecd,df->ecf", arrived, expert_up[0], preferred_element_type=jnp.float32)
    hidden = (jax.nn.silu(gate_part) * up_part).astype(jnp.bfloat16)
    partial_value = jnp.einsum(
        "ecf,fd->ecd", hidden, expert_down[0], preferred_element_type=jnp.float32
    )
    summed = lax.psum_scatter(
        partial_value.astype(jnp.bfloat16), "tp", scatter_dimension=2, tiled=True
    )
    returned = lax.all_to_all(summed, "ep", split_axis=0, concat_axis=0, tiled=True)
    routed = jnp.dot(
        combine,
        returned.reshape(slots_all, columns).astype(jnp.float32),
        precision=lax.Precision.HIGHEST,
    )
    shared_hidden = (
        jax.nn.silu(jnp.dot(whole, shared_gate, preferred_element_type=jnp.float32))
        * jnp.dot(whole, shared_up, preferred_element_type=jnp.float32)
    ).astype(jnp.bfloat16)
    shared_term = jnp.dot(shared_hidden, shared_down, preferred_element_type=jnp.float32)
    shared = lax.psum_scatter(
        shared_term.astype(jnp.bfloat16), "tp", scatter_dimension=1, tiled=True
    ).astype(jnp.float32)
    after = RESIDUAL_SCALE * normed.astype(jnp.float32) + routed + shared
    final_totals, final_squares = lax.psum(
        (jnp.sum(after, axis=1), jnp.sum(after * after, axis=1)), "tp"
    )
    return normalize(
        final_totals[:, None], final_squares[:, None], full_width, after, norm2_gain, norm2_bias
    ).astype(jnp.bfloat16)


def solution(mesh):
    in_specs = (
        P("ep", "tp"),
        P(("ep", "tp"), None),
        P(("ep", "tp"), None, None),
        P(("ep", "tp"), None, None),
        P(("ep", "tp")),
        P(),
        P(None, "tp"),
        P("tp"),
        P("tp"),
        P("ep", None),
        P("ep", None),
        P("ep", None, "tp"),
        P("ep", None, "tp"),
        P("ep", "tp", None),
        P(None, "tp"),
        P(None, "tp"),
        P("tp", None),
        P("tp"),
        P("tp"),
    )
    out_specs = P("ep", "tp")
    ne = mesh.shape["ep"]
    fits = mesh.shape["tp"] == 2 and ne in (2, 4, 8, 16, 32)
    step = functools.partial(paired, ne) if fits else body
    return jax.shard_map(step, mesh=mesh, in_specs=in_specs, out_specs=out_specs, check_vma=False)
```
